32 devices in a mesh: sp: 8 (over z, core), tp: 4 (over y, x).
Axes of the slice: x: 2, y: 2, z: 4, core: 2. Of those that a mesh axis runs over, the one named last changes fastest.
Arguments:
- tokens: bfloat16 [6144, 2048], P('sp', 'tp'), may hold values from -26 to 26, as said below
- mix_gain: bfloat16 [2, 2048], replicated, may hold values from 0.099609375 to 1.8984375
- x_weight: bfloat16 [2, 2048, 1024], P(None, 'sp', 'tp'), may hold values from -0.125 to 0.125
- gate_weight: bfloat16 [2, 2048, 1024], P(None, 'sp', 'tp'), may hold values from -0.125 to 0.125
- conv_taps: bfloat16 [2, 4, 1024], P(None, None, 'tp'), may hold values from -3 to 3
- a_maps: bfloat16 [2, 16, 64, 64], P(None, 'tp'), may hold values from -0.75 to 0.75
- i_maps: bfloat16 [2, 16, 64, 64], P(None, 'tp'), may hold values from -0.75 to 0.75
- decay_rate: float32 [2, 1024], P(None, 'tp'), as said below
- pace: float32 [6144], P('sp'), may hold values from 0.35 to 2.8, as said below
- jumps: float32 [6144], P('sp'), may hold values from -0.7 to 0, as said below
- out_gain: bfloat16 [2, 1024], P(None, 'tp'), may hold values from 0.099609375 to 1.8984375
- out_weight: bfloat16 [2, 1024, 2048], P(None, 'sp', 'tp'), may hold values from -0.1875 to 0.1875
Outputs:
- stream: bfloat16 [6144, 2048], P('sp', 'tp')
The draws below stay inside these ranges and needn't reach their ends.
Inputs may be any that keep to these rules, and one draw needn't show every extreme that they name: `tokens`: random-looking real values; feature scales differ along the features. `decay_rate`: positive. `pace`: positive. `jumps`: zero or negative.
All inputs are finite; a program needn't handle non-finite values.
Results may differ from the reference program's by a relative error of at most 0.01.
Values may be sent and summed in bfloat16 or wider, within the bound.
No kernel may reach another device: no remote copies, remote signals or barrier semaphores. Data moves between devices by JAX's collectives and lax.ppermute only.
A program may use at most 64 MiB of HBM per device.

```python
import math
import jax
import jax.numpy as jnp
from jax import lax

D = 2048
D_REC = 1024
HEAD = 64
WIDTH = 4
LAYERS = 2
TOK_DEV = 768
TOKENS = 6144
HEADS = 16


def draw_tokens(key, part):
    first = jax.random.fold_in(key, 11)
    second = jax.random.fold_in(key, 12)
    ramp = jnp.exp(jnp.linspace(0.0, math.log(3.0), D)).astype(jnp.float32)
    rough = jnp.exp(jax.random.uniform(second, (D,), jnp.float32, -0.35, 0.35))
    values = jnp.clip(jax.random.normal(first, (TOKENS, D), jnp.float32), -6.0, 6.0)
    return (values * ramp[None, :] * rough[None, :]).astype(jnp.bfloat16)


def draw_decay_rate(key, part):
    first = jax.random.fold_in(key, 21)
    second = jax.random.fold_in(key, 22)
    third = jax.random.fold_in(key, 23)
    share = 0.5
    fast = jax.random.uniform(first, (LAYERS, D_REC), jnp.float32) < share
    quick = jnp.exp(jax.random.uniform(second, (LAYERS, D_REC), jnp.float32, math.log(0.004), math.log(0.012)))
    slow = jnp.exp(jax.random.uniform(third, (LAYERS, D_REC), jnp.float32, math.log(0.02), math.log(0.1))) / TOKENS
    return jnp.where(fast, quick, slow).astype(jnp.float32)


def draw_pace(key, part):
    first = jax.random.fold_in(key, 31)
    second = jax.random.fold_in(key, 32)
    blocks = TOKENS // TOK_DEV
    block_factor = jnp.exp(jax.random.uniform(first, (blocks,), jnp.float32, math.log(0.5), math.log(2.0)))
    fine = jnp.exp(jax.random.uniform(second, (TOKENS,), jnp.float32, math.log(0.7), math.log(1.4)))
    return (jnp.repeat(block_factor, TOK_DEV) * fine).astype(jnp.float32)


def draw_jumps(key, part):
    first = jax.random.fold_in(key, 41)
    second = jax.random.fold_in(key, 42)
    spots = jax.random.randint(first, (6,), 0, TOKENS)
    sizes = jnp.log(jax.random.uniform(second, (6,), jnp.float32, 0.5, 0.8))
    return jnp.zeros((TOKENS,), jnp.float32).at[spots].set(sizes)


def levels(rng, shape, cuts, smallest, top_value):
    loudness = 1.0
    for position, parts in cuts:
        heights = jax.random.uniform(jax.random.fold_in(jax.random.fold_in(rng, 6), position), (parts,), jnp.float32, smallest / len(cuts), top_value / len(cuts))
        loudness = loudness * jnp.repeat(jnp.exp(heights), shape[position] // parts).reshape((-1,) + (1,) * (len(shape) - 1 - position))
    return loudness


def normal_values(stream_key, extent, deviation, limit, split=(), held_as=jnp.bfloat16):
    result = jax.random.normal(stream_key, extent, jnp.float32) * deviation
    if len(split) > 0:
        result = levels(stream_key, extent, split, -0.22, 0.18) * result
    return jnp.clip(result, min=-limit, max=limit).astype(held_as)


def setup_inputs(seed: int = 0) -> dict:
    seeds = jax.random.split(jax.random.key(seed), 13)
    return {
        "tokens": draw_tokens(jax.random.fold_in(seeds[12], 71), 0),
        "mix_gain": jnp.clip(1.0 + 0.18 * jax.random.normal(seeds[1], (LAYERS, D), jnp.float32), 0.099609375, 1.8984375).astype(jnp.bfloat16),
        "x_weight": normal_values(seeds[2], (LAYERS, D, D_REC), D ** -0.5, 0.125, ((1, 8), (2, 4))),
        "gate_weight": normal_values(seeds[3], (LAYERS, D, D_REC), D ** -0.5, 0.125, ((1, 8), (2, 4))),
        "conv_taps": normal_values(seeds[4], (LAYERS, WIDTH, D_REC), WIDTH ** -0.5, 3.0, ((2, 4),)),
        "a_maps": normal_values(seeds[5], (LAYERS, HEADS, HEAD, HEAD), HEAD ** -0.5, 0.75, ((1, 4),)),
        "i_maps": normal_values(seeds[6], (LAYERS, HEADS, HEAD, HEAD), HEAD ** -0.5, 0.75, ((1, 4),)),
        "decay_rate": draw_decay_rate(jax.random.fold_in(seeds[12], 71), 0),
        "pace": draw_pace(jax.random.fold_in(seeds[12], 71), 0),
        "jumps": draw_jumps(jax.random.fold_in(seeds[12], 71), 0),
        "out_gain": jnp.clip(1.0 + 0.18 * jax.random.normal(seeds[10], (LAYERS, D_REC), jnp.float32), 0.099609375, 1.8984375).astype(jnp.bfloat16),
        "out_weight": normal_values(seeds[11], (LAYERS, D_REC, D), D_REC ** -0.5, 0.1875, ((1, 8), (2, 4))),
    }


EPS = 1e-06
GATE_C = 8.0

def combine(first, second):
    return (first[0] * second[0], second[0] * first[1] + second[1])

def reference(tokens, mix_gain, x_weight, gate_weight, conv_taps, a_maps, i_maps, decay_rate, pace, jumps, out_gain, out_weight):
    f32 = jnp.float32
    stream = tokens
    for layer in range(LAYERS):
        xf = stream.astype(f32)
        normed = (xf * lax.rsqrt(lax.optimization_barrier(jnp.mean(xf * xf, axis=1, keepdims=True)) + EPS) * mix_gain[layer].astype(f32)).astype(jnp.bfloat16)
        xr = jnp.dot(normed, x_weight[layer], preferred_element_type=f32).astype(jnp.bfloat16)
        gr = jnp.dot(normed, gate_weight[layer], preferred_element_type=f32).astype(jnp.bfloat16)
        padded = jnp.pad(xr, ((WIDTH - 1, 0), (0, 0))).astype(f32)
        taps = conv_taps[layer].astype(f32)
        conv = jnp.zeros((TOKENS, D_REC), f32)
        for k in range(WIDTH):
            conv = conv + taps[k][None, :] * padded[k:k + TOKENS]
        xc = conv.astype(jnp.bfloat16)
        grouped = xc.astype(f32).reshape(TOKENS, HEADS, HEAD)
        rgate = jax.nn.sigmoid(jnp.einsum('thi,hij->thj', grouped, a_maps[layer].astype(f32)).reshape(TOKENS, D_REC))
        igate = jax.nn.sigmoid(jnp.einsum('thi,hij->thj', grouped, i_maps[layer].astype(f32)).reshape(TOKENS, D_REC))
        log_a = -GATE_C * rgate * decay_rate[layer][None, :] * pace[:, None] + jumps[:, None]
        decay = jnp.exp(log_a)
        drive = jnp.sqrt(-jnp.expm1(2.0 * log_a)) * igate * xc.astype(f32)
        _, state = lax.associative_scan(combine, (decay, drive), axis=0)
        rec = state * jax.nn.gelu(gr.astype(f32))
        scale = lax.rsqrt(lax.optimization_barrier(jnp.mean(rec * rec, axis=1, keepdims=True)) + EPS)
        mixed = (rec * out_gain[layer].astype(f32)[None, :]).astype(jnp.bfloat16)
        stream = (xf + jnp.dot(mixed, out_weight[layer], preferred_element_type=f32) * scale).astype(jnp.bfloat16)
    return stream
```

```python
import functools

import jax
import jax.numpy as jnp
from jax import lax
from jax.experimental import pallas as pl
from jax.experimental.pallas import tpu as pltpu
from jax.sharding import PartitionSpec as P

EPS = 1e-06
GATE_C = 8.0
SEGS = 8
HALO = 8
F32 = jnp.float32
BF16 = jnp.bfloat16


VMEM = pl.BlockSpec(memory_space=pltpu.VMEM)
SMEM = pl.BlockSpec(memory_space=pltpu.SMEM)


def call(body, name, outs, n_in, scratch=(), flops=0, nbytes=0, limit=56 << 20):
    return pl.pallas_call(
        body,
        out_shape=outs,
        in_specs=[SMEM] + [VMEM] * (n_in - 1),
        out_specs=jax.tree.map(lambda _: VMEM, outs),
        scratch_shapes=list(scratch),
        compiler_params=pltpu.CompilerParams(vmem_limit_bytes=limit),
        cost_estimate=pl.CostEstimate(flops=flops, bytes_accessed=nbytes, transcendentals=0),
        name=name,
    )


def sds(shape, dtype):
    return jax.ShapeDtypeStruct(shape, dtype)


LANES = 128


def tiles(chans):
    return -(-chans // LANES)


def by_tile(rows, chans):
    return pltpu.VMEM((tiles(chans), rows, LANES), F32)


def put_rows(ref, at, vals):
    chans = vals.shape[1]
    if chans % LANES:
        pad = jnp.zeros((vals.shape[0], -chans % LANES), vals.dtype)
        vals = jnp.concatenate([vals, pad], axis=1)
    for n in range(tiles(chans)):
        ref[n, at, :] = vals[:, n * LANES : (n + 1) * LANES]


def get_rows(ref, at, chans):
    return jnp.concatenate([ref[n, at, :] for n in range(tiles(chans))], axis=1)[:, :chans]


def swap_tp(a, mask):
    n = lax.axis_size("tp")
    return lax.ppermute(a, "tp", [(i, i ^ mask) for i in range(n)])


def swap_core(a):
    n = lax.axis_size("sp")
    return lax.ppermute(a, "sp", [(i, i ^ 1) for i in range(n)])


def along_z(a):
    n = lax.axis_size("sp")
    pairs = [(i, i + 2) for i in range(0, n - 2, 2)] + [(i + 2, i) for i in range(1, n - 2, 2)]
    return lax.ppermute(a, "sp", pairs)


def up_z(a, by):
    n = lax.axis_size("sp")
    return lax.ppermute(a, "sp", [(i, i + 2 * by) for i in range(n - 2 * by)])


def gather_tp(top, low):
    n = lax.axis_size("tp")
    bits = [1 << b for b in range(n.bit_length() - 1)]
    out = []
    for part, order in ((top, bits), (low, bits[::-1])):
        held = {0: part}
        for bit in order:
            for mask in list(held):
                held[mask | bit] = swap_tp(held[mask], bit)
        out.append([held[m] for m in range(n)])
    return out


def halo_from_behind(rows):
    n, m = lax.axis_size("sp"), lax.axis_size("tp")
    return [
        lax.ppermute(
            rows,
            ("sp", "tp"),
            [(s * m + t, (s + 1) * m + (t ^ k)) for s in range(n - 1) for t in range(m)],
        )
        for k in range(m)
    ]


def spread_weights(shard):
    other = swap_core(shard)
    slot = jnp.concatenate([shard, other], axis=0)
    mine = []
    for _ in range(lax.axis_size("sp") // 2 - 1):
        slot = along_z(slot)
        mine.append(slot)
    return [shard, other] + mine + [swap_core(a) for a in mine]


def assemble_body(steps, spans, idx, *refs):
    n_in = 2 + 2 * steps
    ins, outs = refs[:n_in], refs[n_in:]
    pos, core = idx[0], idx[1]
    z = pos // 2
    sp = 2 * (steps + 1)
    rows = ins[0].shape[0]

    def put(src, off, owner):
        base = 0
        for out, span in zip(outs, spans):
            where = pl.multiple_of(owner * span, span)
            out[pl.ds(where, span), :] = src[off + base : off + base + span, :]
            base += span

    put(ins[0], 0, pos)
    put(ins[1], 0, pos + 1 - 2 * core)
    for k in range(1, steps + 1):
        for src, far, first in (
            (ins[1 + k], z - k + 2 * k * core, core),
            (ins[1 + steps + k], z + k - 2 * k * core, 1 - core),
        ):

            @pl.when(jnp.logical_and(far >= 0, far < sp // 2))
            def _():
                put(src, 0, 2 * far + first)
                put(src, rows, 2 * far + 1 - first)


def assemble(idx, pieces, spans):
    steps = (len(pieces) - 2) // 2
    sp = 2 * (steps + 1)
    cols = pieces[0].shape[1]
    outs = [sds((sp * s, cols), BF16) for s in spans]
    nbytes = 2 * sp * sum(spans) * cols * 2
    return call(
        functools.partial(assemble_body, steps, spans),
        "assemble",
        outs,
        1 + len(pieces),
        nbytes=nbytes,
        flops=nbytes,
    )(idx, *pieces)


def widen(vals, me):
    while vals[0].shape[1] % LANES:
        odd = lax.rem(me, 2) == 1
        pairs = zip(vals[::2], vals[1::2])
        vals = [
            jnp.concatenate([jnp.where(odd, b, a), jnp.where(odd, a, b)], axis=1) for a, b in pairs
        ]
        me = me // 2
    return vals, me


def sigmoid(v):
    return 0.5 * jnp.tanh(0.5 * v) + 0.5


def gelu(v):
    inner = 0.7978845608028654 * (v + 0.044715 * (v * v * v))
    return 0.5 * v * (1.0 + jnp.tanh(inner))


def neg_expm1(y, ey):
    series = 1.0 + y * (1.0 / 6.0)
    for n in (5.0, 4.0, 3.0, 2.0):
        series = 1.0 + y * (1.0 / n) * series
    return jnp.where(y > -0.3, -y * series, 1.0 - ey)


def front_body(n_tp, idx, *refs):
    tops, lows, halos = refs[:n_tp], refs[n_tp : 2 * n_tp], refs[2 * n_tp : 3 * n_tp]
    gain, w, taps, maps, rate, pace, jumps = refs[3 * n_tp : 3 * n_tp + 7]
    h_ref, p_ref, g_ref, seg_ref, tot_ref = refs[3 * n_tp + 7 : 3 * n_tp + 12]
    normed, hnormed, xr_s, gr_s = refs[3 * n_tp + 12 :]
    me = idx[2]
    half, width = tops[0].shape
    tok = 2 * half
    steps = tok // SEGS
    chans = rate.shape[1]
    d = width * n_tp

    def norm_rows(srcs, rows, dst, at, pick):
        total = 0.0
        for k in range(n_tp):
            v = srcs[k][pick].astype(F32)
            total = total + jnp.sum(v * v, axis=1, keepdims=True)
        scale = lax.rsqrt(total * (1.0 / d) + EPS)
        for k in range(n_tp):
            where = pl.multiple_of((me ^ k) * width, width)
            v = srcs[k][pick].astype(F32)
            out = v * scale * gain[:, pl.ds(where, width)].astype(F32)
            dst[at, pl.ds(where, width)] = out.astype(BF16)

    norm_rows(halos, HALO, hnormed, slice(None), slice(None))
    rim = jnp.dot(hnormed[...], w[:, :chans], preferred_element_type=F32).astype(BF16).astype(F32)

    block = 64
    for side, srcs in enumerate((tops, lows)):

        def norm_block(i, _):
            at = pl.multiple_of(i * block, block)
            norm_rows(srcs, block, normed, pl.ds(at, block), pl.ds(at, block))
            return 0

        lax.fori_loop(0, half // block, norm_block, 0)
        proj = jnp.dot(normed[...], w[...], preferred_element_type=F32).astype(BF16).astype(F32)
        for s in range(SEGS // 2):
            rows = proj[s * steps : (s + 1) * steps]
            seg = side * (SEGS // 2) + s
            put_rows(xr_s, pl.ds(3 * SEGS + seg, steps, SEGS), rows[:, :chans])
            put_rows(gr_s, pl.ds(seg, steps, SEGS), rows[:, chans:])

    top_row = lax.broadcasted_iota(jnp.int32, (SEGS, chans), 0) == 0
    for i in range(3):
        tail = get_rows(xr_s, pl.ds((steps + i) * SEGS, SEGS), chans)
        tail = pltpu.roll(tail, 1, 0)
        first = jnp.broadcast_to(rim[HALO - 3 + i : HALO - 2 + i], (SEGS, chans))
        put_rows(xr_s, pl.ds(i * SEGS, SEGS), jnp.where(top_row, first, tail))

    tapf = taps[...].astype(F32)
    slope = rate[...] * (-GATE_C)
    chunk = 16 * SEGS

    def one(i, carry):
        h, p = carry
        base = pl.multiple_of(i * chunk, chunk)
        conv = jnp.zeros((chunk, chans), F32)
        for k in range(4):
            conv = conv + tapf[k : k + 1] * get_rows(xr_s, pl.ds(base + k * SEGS, chunk), chans)
        xcb = conv.astype(BF16)
        xc = xcb.astype(F32)
        gates = jnp.dot(xcb, maps[...], preferred_element_type=F32)
        rg = sigmoid(gates[:, :chans])
        ig = sigmoid(gates[:, chans:])
        log_a = rg * slope * pace[pl.ds(base, chunk), :] + jumps[pl.ds(base, chunk), :]
        a = jnp.exp(log_a)
        b = jnp.sqrt(neg_expm1(2.0 * log_a, a * a)) * ig * xc
        g_ref[pl.ds(base, chunk), :] = gelu(get_rows(gr_s, pl.ds(base, chunk), chans))
        for j in range(chunk // SEGS):
            aj = a[j * SEGS : (j + 1) * SEGS]
            h = aj * h + b[j * SEGS : (j + 1) * SEGS]
            p = p * aj
            h_ref[pl.ds(base + j * SEGS, SEGS), :] = h
            p_ref[pl.ds(base + j * SEGS, SEGS), :] = p
        return h, p

    h, p = lax.fori_loop(
        0,
        tok // chunk,
        one,
        (jnp.zeros((SEGS, chans), F32), jnp.ones((SEGS, chans), F32)),
    )
    run_p, run_s = jnp.ones((1, chans), F32), jnp.zeros((1, chans), F32)
    for s in range(SEGS):
        seg_ref[pl.ds(s, 1), :] = run_p
        seg_ref[pl.ds(SEGS + s, 1), :] = run_s
        run_s = p[s : s + 1] * run_s + h[s : s + 1]
        run_p = p[s : s + 1] * run_p
    tot_ref[0:1, :] = run_p
    tot_ref[1:2, :] = run_s


def front(idx, tops, lows, halos, gain, w, taps, maps, rate, pace, jumps):
    n_tp = len(tops)
    tok = 2 * tops[0].shape[0]
    d = n_tp * tops[0].shape[1]
    chans = rate.shape[1]
    outs = [
        sds((tok, chans), F32),
        sds((tok, chans), F32),
        sds((tok, chans), F32),
        sds((2 * SEGS, chans), F32),
        sds((2, chans), F32),
    ]
    scratch = [
        pltpu.VMEM((tok // 2, d), BF16),
        pltpu.VMEM((HALO, d), BF16),
        by_tile(tok + 3 * SEGS, chans),
        by_tile(tok, chans),
    ]
    args = [idx, *tops, *lows, *halos, gain, w, taps, maps, rate, pace, jumps]
    return call(
        functools.partial(front_body, n_tp),
        "front",
        outs,
        len(args),
        scratch,
        flops=4 * tok * d * chans * 2,
        nbytes=8 << 20,
    )(*args)


def fix_body(hops, idx, *refs):
    h_ref, p_ref, g_ref, seg_ref, pair_ref, gain = refs[:6]
    behind = refs[6 : 6 + hops]
    top_ref, low_ref = refs[6 + hops : 8 + hops]
    mixed = refs[8 + hops]
    core = idx[1]
    tok, chans = h_ref.shape
    steps = tok // SEGS
    inc = jnp.zeros((1, chans), F32)
    for ref in behind[::-1]:
        inc = ref[0:1, :] * inc + ref[1:2, :]
    inc = jnp.where(core == 1, pair_ref[0:1, :] * inc + pair_ref[1:2, :], inc)
    carry = seg_ref[SEGS:, :] + seg_ref[:SEGS, :] * inc
    scale = gain[...].astype(F32)
    chunk = 16 * SEGS
    many = jnp.concatenate([carry] * (chunk // SEGS), axis=0)

    def one(i, _):
        at = pl.ds(pl.multiple_of(i * chunk, chunk), chunk)
        rec = (h_ref[at, :] + p_ref[at, :] * many) * g_ref[at, :]
        put_rows(mixed, at, rec * scale)
        return 0

    lax.fori_loop(0, tok // chunk, one, 0)
    for s in range(SEGS):
        out = top_ref if s < SEGS // 2 else low_ref
        at = (s % (SEGS // 2)) * steps
        out[pl.ds(at, steps), :] = get_rows(mixed, pl.ds(s, steps, SEGS), chans).astype(BF16)


def fix(idx, h, p, g, seg, pair, gain, behind):
    tok, chans = h.shape
    outs = [sds((tok // 2, chans), BF16)] * 2
    args = [idx, h, p, g, seg, pair, gain, *behind]
    return call(
        functools.partial(fix_body, len(behind)),
        "fix",
        outs,
        len(args),
        [by_tile(tok, chans)],
        flops=tok * chans * 1000,
        nbytes=4 << 20,
    )(*args)


def back_body(n_tp, last, idx, *refs):
    tops, lows, gains = refs[:n_tp], refs[n_tp : 2 * n_tp], refs[2 * n_tp : 3 * n_tp]
    rest = refs[3 * n_tp :]
    w, old_top, old_low = rest[:3]
    outs = rest[3:-2]
    full, inv = rest[-2:]
    me = idx[2]
    half, width = tops[0].shape
    rec_d = width * n_tp

    def place(srcs, dst, at):
        vals, group = widen([r[...] for r in srcs], me)
        span = vals[0].shape[1]
        for k, v in enumerate(vals):
            dst[at, pl.ds(pl.multiple_of((group ^ k) * span, span), span)] = v

    place(gains, inv, slice(None))
    inv[...] = 1.0 / (inv[...] * inv[...])
    place(tops, full, slice(0, half))
    place(lows, full, slice(half, 2 * half))
    block = half // 2
    for i in range(4):
        at = i * block
        m = full[at : at + block, :]
        mf = m.astype(F32)
        squares = jnp.sum(mf * mf * inv[...], axis=1, keepdims=True)
        scale = lax.rsqrt(squares * (1.0 / rec_d) + EPS)
        update = jnp.dot(m, w[...], preferred_element_type=F32)
        old = old_top if i < 2 else old_low
        off = (i % 2) * block
        new = (old[off : off + block, :].astype(F32) + update * scale).astype(BF16)
        if last:
            outs[0][at : at + block, :] = new
        else:
            outs[i // 2][off : off + block, :] = new
            if i == 3:
                outs[2][...] = new[block - HALO :]


def back(idx, tops, lows, gains, w, old_top, old_low, last):
    n_tp = len(tops)
    half, width = tops[0].shape
    cols = w.shape[1]
    if last:
        outs = [sds((2 * half, cols), BF16)]
    else:
        outs = [sds((half, cols), BF16)] * 2 + [sds((HALO, cols), BF16)]
    args = [idx, *tops, *lows, *gains, w, old_top, old_low]
    return call(
        functools.partial(back_body, n_tp, last),
        "back",
        outs,
        len(args),
        [pltpu.VMEM((2 * half, n_tp * width), BF16), pltpu.VMEM((1, n_tp * width), F32)],
        flops=4 * half * n_tp * width * cols,
        nbytes=4 << 20,
    )(*args)


def block_diagonal(maps):
    heads, n, _ = maps.shape
    eye = jnp.eye(heads, dtype=maps.dtype)
    return (eye[:, None, :, None] * maps[:, :, None, :]).reshape(heads * n, heads * n)


def body(
    tokens,
    mix_gain,
    x_weight,
    gate_weight,
    conv_taps,
    a_maps,
    i_maps,
    decay_rate,
    pace,
    jumps,
    out_gain,
    out_weight,
):
    layers = mix_gain.shape[0]
    tok, width = tokens.shape
    half, steps = tok // 2, tok // SEGS
    pos, me = lax.axis_index("sp"), lax.axis_index("tp")
    core = pos % 2
    idx = jnp.stack([pos, core, me]).astype(jnp.int32)
    n_tp = lax.axis_size("tp")
    hops = lax.axis_size("sp") // 2 - 1

    def in_steps(v):
        return v.reshape(SEGS, steps).T.reshape(tok, 1)

    xg_rows, o_rows = x_weight.shape[1], out_weight.shape[1]
    xg = [jnp.concatenate([x_weight[l], gate_weight[l]], axis=1) for l in range(layers)]

    top, low, halo = tokens[:half], tokens[half:], tokens[tok - HALO :]
    tops, lows = gather_tp(top, low)
    w_in, w_out = [None] * layers, [None] * layers
    (w_in[0],) = assemble(idx, spread_weights(xg[0]), [xg_rows])
    halos = halo_from_behind(halo)
    gains = [swap_tp(out_gain, k) if k else out_gain for k in range(n_tp)]
    rest, spans = [out_weight[0]], [o_rows]
    for l in range(1, layers):
        rest += [xg[l], out_weight[l]]
        spans += [xg_rows, o_rows]
    got = assemble(idx, spread_weights(jnp.concatenate(rest, axis=0)), spans)
    w_out[0] = got[0]
    for l in range(1, layers):
        w_in[l], w_out[l] = got[2 * l - 1], got[2 * l]

    pace_s, jumps_s = in_steps(pace), in_steps(jumps)
    for l in range(layers):
        maps = jnp.concatenate([block_diagonal(a_maps[l]), block_diagonal(i_maps[l])], axis=1)
        h, p, g, seg, tot = front(
            idx,
            tops,
            lows,
            halos,
            mix_gain[l][None, :],
            w_in[l],
            conv_taps[l],
            maps,
            decay_rate[l][None, :],
            pace_s,
            jumps_s,
        )
        pair = swap_core(tot)
        first = jnp.where(core == 0, tot, pair)
        second = jnp.where(core == 0, pair, tot)
        both = jnp.stack([first[0] * second[0], second[0] * first[1] + second[1]])
        behind = [up_z(both, k) for k in range(1, hops + 1)]
        m_top, m_low = fix(idx, h, p, g, seg, pair, out_gain[l][None, :], behind)
        m_tops, m_lows = gather_tp(m_top, m_low)
        last = l == layers - 1
        new = back(
            idx, m_tops, m_lows, [v[l][None, :].astype(F32) for v in gains], w_out[l], top, low, last
        )
        if last:
            return new[0]
        top, low, halo = new
        tops, lows = gather_tp(top, low)
        halos = halo_from_behind(halo)


def solution(mesh):
    in_specs = (
        P("sp", "tp"),
        P(),
        P(None, "sp", "tp"),
        P(None, "sp", "tp"),
        P(None, None, "tp"),
        P(None, "tp", None, None),
        P(None, "tp", None, None),
        P(None, "tp"),
        P("sp"),
        P("sp"),
        P(None, "tp"),
        P(None, "sp", "tp"),
    )
    return jax.shard_map(
        body, mesh=mesh, in_specs=in_specs, out_specs=P("sp", "tp"), check_vma=False
    )
```
